32 devices in a mesh: rep: 2 (over x), fs: 8 (over z, y), tp: 2 (over core).
Axes of the slice: x: 2, y: 2, z: 4, core: 2. Of those that a mesh axis runs over, the one named last changes fastest.
Arguments:
- inputs: bfloat16 [8192, 2048], P(('rep', 'fs')), may hold values from -6 to 6
- cotangent: bfloat16 [8192, 2048], P(('rep', 'fs')), may hold values from -6 to 6
- gate_weight: bfloat16 [2048, 4096], P('fs', 'tp'), may hold values from -0.125 to 0.125
- up_weight: bfloat16 [2048, 4096], P('fs', 'tp'), may hold values from -0.125 to 0.125
- down_weight: bfloat16 [2048, 4096], P('fs', 'tp'), may hold values from -0.09375 to 0.09375
Outputs:
- grad_input: bfloat16 [8192, 2048], P(('rep', 'fs'))
- grad_down: float32 [2048, 4096], P('fs', 'tp')
The draws below stay inside these ranges and needn't reach their ends.
All inputs are finite; a program needn't handle non-finite values.
Results may differ from the reference program's by a relative error of at most 0.014.
Values may be sent and summed in bfloat16 or wider, within the bound.
A program may use at most 128 MiB of HBM per device.

```python
import jax
import jax.numpy as jnp
from jax import lax

D = 2048
FF = 4096
TOK_DEV = 512
TOKENS = 8192
N_TP = 2


def raised(values, key, source, target, shards_of, factor):
    owner, partner = [(jnp.arange(values.shape[axis_at]) // (values.shape[axis_at] // shards_of)).reshape([-1 if axis == axis_at else 1 for axis in range(values.ndim)]) for axis_at in (source, target)]
    chosen = jax.random.permutation(key, shards_of)[partner]
    strong = (owner == chosen) | (owner == (partner + shards_of // 2) % shards_of)
    return jnp.where(strong, factor * values, values)


def shard_levels(stream_key, shape, cuts, low, high):
    loudness, own = 1.0, jax.random.fold_in(stream_key, 6)
    for position, shards_of in cuts:
        draws = jnp.exp(jax.random.uniform(jax.random.fold_in(own, position), (shards_of,), jnp.float32, low / len(cuts), high / len(cuts)))
        loudness = loudness * jnp.repeat(draws, shape[position] // shards_of).reshape([-1 if axis == position else 1 for axis in range(len(shape))])
    return loudness


def normal_values(stream_key, dims, scale, most, split=(), held_as=jnp.bfloat16):
    entries = scale * jax.random.normal(stream_key, dims, jnp.float32)
    if split:
        entries = entries * shard_levels(stream_key, dims, split, -0.22, 0.18)
    return jnp.clip(entries, -most, most).astype(held_as)


def heavy_noise(rng, extent, width, most, cuts, heavy, kind=jnp.bfloat16):
    result = width * jax.random.normal(rng, extent, jnp.float32)
    if cuts:
        result = result * shard_levels(rng, extent, cuts, -0.22, 0.18)
    return jnp.clip(raised(result, jax.random.fold_in(rng, 3), *heavy), -most, most).astype(kind)


def setup_inputs(seed: int = 0) -> dict:
    splits = jax.random.split(jax.random.key(seed), 6)
    inputs = normal_values(splits[0], (TOKENS, D), 1.0, 6.0, ((0, 16),))
    cotangent = heavy_noise(splits[1], (TOKENS, D), 1.0, 6.0, ((0, 16),), (0, 1, 16, 2.0))
    gate_weight = normal_values(splits[2], (D, FF), D ** -0.5, 0.125, ((0, 8), (1, 2)))
    up_weight = normal_values(splits[3], (D, FF), D ** -0.5, 0.125, ((0, 8), (1, 2)))
    down_weight = normal_values(splits[4], (D, FF), FF ** -0.5, 0.09375, ((0, 8), (1, 2)))
    return dict(inputs=inputs, cotangent=cotangent, gate_weight=gate_weight, up_weight=up_weight, down_weight=down_weight)


def reference(inputs, cotangent, gate_weight, up_weight, down_weight):
    hid_width = FF // N_TP
    contract = (((1,), (1,)), ((), ()))
    contract_tok = (((0,), (0,)), ((), ()))

    def one_block(grad_acc, block_index):
        row_start = (block_index * TOK_DEV).astype(jnp.int32)
        in_rows = lax.dynamic_slice_in_dim(inputs, row_start, TOK_DEV, 0)
        cot_rows = lax.dynamic_slice_in_dim(cotangent, row_start, TOK_DEV, 0)
        gate_val = jnp.dot(in_rows, gate_weight, preferred_element_type=jnp.float32)
        up_val = jnp.dot(in_rows, up_weight, preferred_element_type=jnp.float32)
        sigmoid_gate = jax.nn.sigmoid(gate_val)
        active = gate_val * sigmoid_gate
        hidden = (active * up_val).astype(jnp.bfloat16)
        grad_hidden = jnp.dot(cot_rows, down_weight, preferred_element_type=jnp.float32)
        grad_gate = (grad_hidden * up_val * sigmoid_gate * (1.0 + gate_val * (1.0 - sigmoid_gate))).astype(jnp.bfloat16)
        grad_up = (grad_hidden * active).astype(jnp.bfloat16)
        total = jnp.zeros((TOK_DEV, D), jnp.float32)
        for blk in range(N_TP):
            lo_col = blk * hid_width
            hi_col = lo_col + hid_width
            piece = lax.dot_general(grad_gate[:, lo_col:hi_col], gate_weight[:, lo_col:hi_col], contract, preferred_element_type=jnp.float32)
            piece = piece + lax.dot_general(grad_up[:, lo_col:hi_col], up_weight[:, lo_col:hi_col], contract, preferred_element_type=jnp.float32)
            rounded = lax.optimization_barrier(piece.astype(jnp.bfloat16))
            total = total + rounded.astype(jnp.float32)
        grad_acc = grad_acc + lax.dot_general(cot_rows, hidden, contract_tok, preferred_element_type=jnp.float32)
        return grad_acc, total.astype(jnp.bfloat16)

    indices = jnp.arange(TOKENS // TOK_DEV, dtype=jnp.int32)
    grad_acc, pieces = lax.scan(one_block, jnp.zeros((D, FF), jnp.float32), indices)
    grad_input = pieces.reshape(TOKENS, D)
    grad_down = grad_acc * (float(TOKENS) ** -0.5)
    return grad_input, grad_down
```

```python
import functools
import math

import jax
import jax.numpy as jnp
from jax import lax
from jax.experimental import pallas as pl
from jax.experimental.pallas import tpu as pltpu
from jax.sharding import PartitionSpec as P

MESH = pl.DeviceIdType.MESH


def gather_kernel(
    line, parts, pieces, toks, cots, w_out, t_out, w_tmp, t_tmp,
    up_s, up_r, dn_s, dn_r, y_s, y_r, tok_s, tok_r, d2d_s, d2d_r, loc, loc2,
):
    r = lax.axis_index("rep")
    f = lax.axis_index("fs")
    t = lax.axis_index("tp")
    z, y = f // 2, f % 2
    rows = toks.shape[0]
    half = rows // 2
    wrows = pieces.shape[2]
    per = pieces.shape[1] // parts
    has_up, has_dn = z < line - 1, z > 0
    up = {"fs": (f + 2) % (2 * line)}
    dn = {"fs": (f + 2 * line - 2) % (2 * line)}
    ypart = {"fs": f + 1 - 2 * y}
    xpart = {"rep": 1 - r}
    core = t % 2
    cpart = {"tp": t + 1 - 2 * core}

    barrier = pltpu.get_barrier_semaphore()

    def greet(dev):
        pl.semaphore_signal(barrier, inc=1, device_id=dev, device_id_type=MESH)

    for dev in (ypart, xpart, cpart, up, dn):
        greet(dev)
    pl.semaphore_wait(barrier, 5)

    def remote(src, dst, s, q, dev):
        return pltpu.make_async_remote_copy(
            src_ref=src, dst_ref=dst, send_sem=s, recv_sem=q,
            device_id=dev, device_id_type=MESH,
        )

    def wblk(k, zz, yy):
        row = pl.multiple_of((2 * zz + yy) * wrows, wrows)
        return w_out.at[pl.ds(k * per, per), pl.ds(row, wrows), :]

    def own(k, yy):
        return pieces.at[yy, pl.ds(k * per, per)]

    def to_y(k):
        return remote(own(k, 1 - y), wblk(k, z, y), y_s.at[k], y_r.at[k], ypart)

    def from_y(k):
        return remote(own(k, 1 - y), wblk(k, z, 1 - y), y_s.at[k], y_r.at[k], ypart)

    def zcopy(up_dir, d, sub, k, zz):
        yy = y if sub == 0 else 1 - y
        src = own(k, y) if (d == 0 and sub == 0) else wblk(k, zz, yy)
        s, q, dev = (up_s, up_r, up) if up_dir else (dn_s, dn_r, dn)
        return remote(src, wblk(k, zz, yy), s.at[d, sub, k], q.at[d, sub, k], dev)

    def pred_send(up_dir, d):
        return (has_up & (z - d >= 0)) if up_dir else (has_dn & (z + d <= line - 1))

    def src_z(up_dir, d):
        return jnp.maximum(z - d, 0) if up_dir else jnp.minimum(z + d, line - 1)

    def send(up_dir, d, sub, k):
        @pl.when(pred_send(up_dir, d))
        def _():
            zcopy(up_dir, d, sub, k, src_z(up_dir, d)).start()

    def await_send(up_dir, d, sub, k):
        @pl.when(pred_send(up_dir, d))
        def _():
            zcopy(up_dir, d, sub, k, src_z(up_dir, d)).wait_send()

    def await_recv(up_dir, d, sub, k):
        ok = (z - d - 1 >= 0) if up_dir else (z + d + 1 <= line - 1)

        @pl.when(ok)
        def _():
            zcopy(up_dir, d, sub, k, src_z(up_dir, d + 1)).wait_recv()

    def tblk(j, rr, yy, c):
        row = pl.multiple_of((2 * rr + yy) * rows + c * half, half)
        return t_out.at[j, pl.ds(row, half), :]

    def mine(j):
        src = toks if j == 0 else cots
        return src.at[pl.ds(pl.multiple_of(core * half, half), half), :]

    def tcopy(i, landing):
        j = (0, 1, 0, 1, 0, 1)[i]
        dev = xpart if i in (0, 1, 5) else ypart
        if landing:
            rr = (1 - r, 1 - r, r, r, 1 - r, 1 - r)[i]
            yy = (y, y, 1 - y, 1 - y, 1 - y, 1 - y)[i]
            src = dst = tblk(j, rr, yy, core)
        else:
            rr = (r, r, r, r, 1 - r, r)[i]
            yy = (y, y, y, y, y, 1 - y)[i]
            dst = tblk(j, rr, yy, core)
            src = mine(j) if i < 4 else dst
        return remote(src, dst, tok_s.at[i], tok_r.at[i], dev)

    def dcopy(i, c):
        j = (0, 1, 0, 1, 0, 1)[i]
        rr = (1 - r, 1 - r, r, r, 1 - r, 1 - r)[i]
        yy = (y, y, 1 - y, 1 - y, 1 - y, 1 - y)[i]
        blk = tblk(j, rr, yy, c)
        return remote(blk, blk, d2d_s.at[i], d2d_r.at[i], cpart)

    loads = [
        pltpu.make_async_copy(pieces.at[y], w_tmp, loc.at[0]),
        pltpu.make_async_copy(toks, t_tmp.at[0], loc.at[1]),
        pltpu.make_async_copy(cots, t_tmp.at[1], loc.at[2]),
    ]
    trow = pl.multiple_of((2 * r + y) * rows, rows)
    wrow = pl.multiple_of(f * wrows, wrows)
    stores = [
        pltpu.make_async_copy(w_tmp, w_out.at[:, pl.ds(wrow, wrows), :], loc2.at[0]),
        pltpu.make_async_copy(t_tmp.at[0], t_out.at[0, pl.ds(trow, rows), :], loc2.at[1]),
        pltpu.make_async_copy(t_tmp.at[1], t_out.at[1, pl.ds(trow, rows), :], loc2.at[2]),
    ]

    for k in range(parts):
        to_y(k).start()
        send(True, 0, 0, k)
        send(False, 0, 0, k)
    for i in (0, 1, 3, 2):
        tcopy(i, False).start()
    for copy in loads:
        copy.start()
    for load, store in zip(loads, stores):
        load.wait()
        store.start()
    for k in range(parts):
        from_y(k).wait_recv()
        send(True, 0, 1, k)
        send(False, 0, 1, k)

    def event(i):
        tcopy(i, True).wait_recv()
        if i == 0:
            tcopy(4, False).start()
        if i == 3:
            tcopy(5, False).start()
        dcopy(i, core).start()

    events = [0, 3, 1, 2, 5, 4]
    for d in range(line - 1):
        for sub in range(2):
            if events:
                event(events.pop(0))
            for k in range(parts):
                for up_dir in (True, False):
                    await_recv(up_dir, d, sub, k)
                    if d + 1 < line - 1:
                        send(up_dir, d + 1, sub, k)
    for i in events:
        event(i)
    for i in range(6):
        dcopy(i, 1 - core).wait_recv()
        dcopy(i, core).wait_send()
        tcopy(i, False).wait_send()
    for k in range(parts):
        to_y(k).wait_send()
        for d in range(line - 1):
            for sub in range(2):
                await_send(True, d, sub, k)
                await_send(False, d, sub, k)
    for store in stores:
        store.wait()


def gather(pieces, toks, cots):
    line = lax.axis_size("fs") // 2
    kinds, wrows, width = pieces.shape[1:]
    parts = kinds if line <= 4 else 1
    dma = pltpu.SemaphoreType.DMA
    zsem = dma((line - 1, 2, parts))
    anyspec = pl.BlockSpec(memory_space=pl.ANY)
    return pl.pallas_call(
        functools.partial(gather_kernel, line, parts),
        out_shape=(
            jax.ShapeDtypeStruct((kinds, 2 * line * wrows, width), pieces.dtype),
            jax.ShapeDtypeStruct((2, 4 * toks.shape[0], toks.shape[1]), toks.dtype),
        ),
        in_specs=[anyspec] * 3,
        out_specs=(anyspec, anyspec),
        scratch_shapes=[
            pltpu.VMEM(pieces.shape[1:], pieces.dtype),
            pltpu.VMEM((2,) + toks.shape, toks.dtype),
            zsem, zsem, zsem, zsem,
            dma((parts,)), dma((parts,)),
            dma((6,)), dma((6,)), dma((6,)), dma((6,)),
            dma((3,)), dma((3,)),
        ],
        compiler_params=pltpu.CompilerParams(collective_id=0, has_side_effects=True),
        name="gather_all",
    )(pieces, toks, cots)


def on_device(inputs, cotangent, gate_weight, up_weight, down_weight):
    tok_rows = inputs.shape[0]
    fs_size = lax.axis_size("fs")
    rep_size = lax.axis_size("rep")
    contract = (((1,), (1,)), ((), ()))
    contract_tok = (((0,), (0,)), ((), ()))
    width = gate_weight.shape[1] // 4
    r = lax.axis_index("rep")
    y = lax.axis_index("fs") % 2

    def piece(side):
        return jnp.stack([
            lax.dynamic_slice_in_dim(weight, (2 * r + side) * width, width, 1)
            for weight in (gate_weight, up_weight, down_weight)
        ])

    weights, tokens = gather(jnp.stack([piece(0), piece(1)]), inputs, cotangent)
    gate_full, up_full, down_full = weights[0], weights[1], weights[2]
    gate_val = jnp.dot(tokens[0], gate_full, preferred_element_type=jnp.float32)
    up_val = jnp.dot(tokens[0], up_full, preferred_element_type=jnp.float32)
    grad_hidden = jnp.dot(tokens[1], down_full, preferred_element_type=jnp.float32)
    sigmoid_gate = jax.nn.sigmoid(gate_val)
    active = gate_val * sigmoid_gate
    hidden = (active * up_val).astype(jnp.bfloat16)
    grad_gate = (
        grad_hidden * up_val * sigmoid_gate * (1.0 + gate_val * (1.0 - sigmoid_gate))
    ).astype(jnp.bfloat16)
    grad_up = (grad_hidden * active).astype(jnp.bfloat16)
    grad_scale = 1.0 / math.sqrt(tok_rows * fs_size * rep_size)
    pairs = [[i, i + 1] for i in range(0, fs_size, 2)]
    lines = [list(range(i, fs_size, 2)) for i in range(2)]
    grad_part = lax.dot_general(
        tokens[1], hidden, contract_tok, preferred_element_type=jnp.float32
    )
    shard = lax.psum_scatter(
        grad_part.astype(jnp.bfloat16), "fs", scatter_dimension=0, tiled=True,
        axis_index_groups=lines,
    ).astype(jnp.float32) * grad_scale
    shard = lax.all_to_all(
        shard, "fs", split_axis=0, concat_axis=1, tiled=True, axis_index_groups=pairs
    )
    grad_down = lax.all_gather(shard, "rep", axis=1, tiled=True)
    part = lax.dot_general(
        grad_gate, gate_full, contract, preferred_element_type=jnp.float32
    )
    part = part + lax.dot_general(
        grad_up, up_full, contract, preferred_element_type=jnp.float32
    )
    part = lax.psum_scatter(
        part.astype(jnp.bfloat16), "rep", scatter_dimension=0, tiled=True
    )
    part = lax.psum_scatter(
        part, "fs", scatter_dimension=0, tiled=True, axis_index_groups=pairs
    )
    grad_input = lax.psum(part, "tp")
    return (grad_input, grad_down)


def solution(mesh):
    placed = (
        P(("rep", "fs"), None),
        P(("rep", "fs"), None),
        P("fs", "tp"),
        P("fs", "tp"),
        P("fs", "tp"),
    )
    return jax.shard_map(
        on_device,
        mesh=mesh,
        in_specs=placed,
        out_specs=(P(("rep", "fs"), None), P("fs", "tp")),
        check_vma=False,
    )
```

```python
import functools
import math

import jax
import jax.numpy as jnp
from jax import lax
from jax.experimental import pallas as pl
from jax.experimental.pallas import tpu as pltpu
from jax.sharding import PartitionSpec as P

MESH = pl.DeviceIdType.MESH


def gather_kernel(
    line, parts, pieces, toks, cots, w_out, t_out, w_tmp, t_tmp,
    up_s, up_r, dn_s, dn_r, y_s, y_r, tok_s, tok_r, d2d_s, d2d_r, loc, loc2,
):
    r = lax.axis_index("rep")
    f = lax.axis_index("fs")
    t = lax.axis_index("tp")
    z, y = f // 2, f % 2
    rows = toks.shape[0]
    half = rows // 2
    wrows = pieces.shape[2]
    per = pieces.shape[1] // parts
    has_up, has_dn = z < line - 1, z > 0
    up = {"fs": (f + 2) % (2 * line)}
    dn = {"fs": (f + 2 * line - 2) % (2 * line)}
    ypart = {"fs": f + 1 - 2 * y}
    xpart = {"rep": 1 - r}
    core = t % 2
    cpart = {"tp": t + 1 - 2 * core}

    barrier = pltpu.get_barrier_semaphore()

    def greet(dev):
        pl.semaphore_signal(barrier, inc=1, device_id=dev, device_id_type=MESH)

    for dev in (ypart, xpart, cpart, up, dn):
        greet(dev)
    pl.semaphore_wait(barrier, 5)

    def remote(src, dst, s, q, dev):
        return pltpu.make_async_remote_copy(
            src_ref=src, dst_ref=dst, send_sem=s, recv_sem=q,
            device_id=dev, device_id_type=MESH,
        )

    def wblk(k, zz, yy):
        row = pl.multiple_of((2 * zz + yy) * wrows, wrows)
        return w_out.at[pl.ds(k * per, per), pl.ds(row, wrows), :]

    def own(k, yy):
        return pieces.at[yy, pl.ds(k * per, per)]

    def to_y(k):
        return remote(own(k, 1 - y), wblk(k, z, y), y_s.at[k], y_r.at[k], ypart)

    def from_y(k):
        return remote(own(k, 1 - y), wblk(k, z, 1 - y), y_s.at[k], y_r.at[k], ypart)

    def zcopy(up_dir, d, sub, k, zz):
        yy = y if sub == 0 else 1 - y
        src = own(k, y) if (d == 0 and sub == 0) else wblk(k, zz, yy)
        s, q, dev = (up_s, up_r, up) if up_dir else (dn_s, dn_r, dn)
        return remote(src, wblk(k, zz, yy), s.at[d, sub, k], q.at[d, sub, k], dev)

    def pred_send(up_dir, d):
        return (has_up & (z - d >= 0)) if up_dir else (has_dn & (z + d <= line - 1))

    def src_z(up_dir, d):
        return jnp.maximum(z - d, 0) if up_dir else jnp.minimum(z + d, line - 1)

    def send(up_dir, d, sub, k):
        @pl.when(pred_send(up_dir, d))
        def _():
            zcopy(up_dir, d, sub, k, src_z(up_dir, d)).start()

    def await_send(up_dir, d, sub, k):
        @pl.when(pred_send(up_dir, d))
        def _():
            zcopy(up_dir, d, sub, k, src_z(up_dir, d)).wait_send()

    def await_recv(up_dir, d, sub, k):
        ok = (z - d - 1 >= 0) if up_dir else (z + d + 1 <= line - 1)

        @pl.when(ok)
        def _():
            zcopy(up_dir, d, sub, k, src_z(up_dir, d + 1)).wait_recv()

    def tblk(j, rr, yy, c):
        row = pl.multiple_of((2 * rr + yy) * rows + c * half, half)
        return t_out.at[j, pl.ds(row, half), :]

    def mine(j):
        src = toks if j == 0 else cots
        return src.at[pl.ds(pl.multiple_of(core * half, half), half), :]

    def tcopy(i, landing):
        j = (0, 1, 0, 1, 0, 1)[i]
        dev = xpart if i in (0, 1, 5) else ypart
        if landing:
            rr = (1 - r, 1 - r, r, r, 1 - r, 1 - r)[i]
            yy = (y, y, 1 - y, 1 - y, 1 - y, 1 - y)[i]
            src = dst = tblk(j, rr, yy, core)
        else:
            rr = (r, r, r, r, 1 - r, r)[i]
            yy = (y, y, y, y, y, 1 - y)[i]
            dst = tblk(j, rr, yy, core)
            src = mine(j) if i < 4 else dst
        return remote(src, dst, tok_s.at[i], tok_r.at[i], dev)

    def dcopy(i, c):
        j = (0, 1, 0, 1, 0, 1)[i]
        rr = (1 - r, 1 - r, r, r, 1 - r, 1 - r)[i]
        yy = (y, y, 1 - y, 1 - y, 1 - y, 1 - y)[i]
        blk = tblk(j, rr, yy, c)
        return remote(blk, blk, d2d_s.at[i], d2d_r.at[i], cpart)

    loads = [
        pltpu.make_async_copy(pieces.at[y], w_tmp, loc.at[0]),
        pltpu.make_async_copy(toks, t_tmp.at[0], loc.at[1]),
        pltpu.make_async_copy(cots, t_tmp.at[1], loc.at[2]),
    ]
    trow = pl.multiple_of((2 * r + y) * rows, rows)
    wrow = pl.multiple_of(f * wrows, wrows)
    stores = [
        pltpu.make_async_copy(w_tmp, w_out.at[:, pl.ds(wrow, wrows), :], loc2.at[0]),
        pltpu.make_async_copy(t_tmp.at[0], t_out.at[0, pl.ds(trow, rows), :], loc2.at[1]),
        pltpu.make_async_copy(t_tmp.at[1], t_out.at[1, pl.ds(trow, rows), :], loc2.at[2]),
    ]

    for k in range(parts):
        to_y(k).start()
        send(True, 0, 0, k)
        send(False, 0, 0, k)
    for i in (0, 1, 3, 2):
        tcopy(i, False).start()
    for copy in loads:
        copy.start()
    for load, store in zip(loads, stores):
        load.wait()
        store.start()
    for k in range(parts):
        from_y(k).wait_recv()
        send(True, 0, 1, k)
        send(False, 0, 1, k)

    def event(i):
        tcopy(i, True).wait_recv()
        if i == 0:
            tcopy(4, False).start()
        if i == 3:
            tcopy(5, False).start()
        dcopy(i, core).start()

    events = [0, 3, 1, 2, 5, 4]
    for d in range(line - 1):
        for sub in range(2):
            if events:
                event(events.pop(0))
            for k in range(parts):
                for up_dir in (True, False):
                    await_recv(up_dir, d, sub, k)
                    if d + 1 < line - 1:
                        send(up_dir, d + 1, sub, k)
    for i in events:
        event(i)
    for i in range(6):
        dcopy(i, 1 - core).wait_recv()
        dcopy(i, core).wait_send()
        tcopy(i, False).wait_send()
    for k in range(parts):
        to_y(k).wait_send()
        for d in range(line - 1):
            for sub in range(2):
                await_send(True, d, sub, k)
                await_send(False, d, sub, k)
    for store in stores:
        store.wait()


def gather(pieces, toks, cots):
    line = lax.axis_size("fs") // 2
    kinds, wrows, width = pieces.shape[1:]
    parts = kinds if line <= 4 else 1
    dma = pltpu.SemaphoreType.DMA
    zsem = dma((line - 1, 2, parts))
    anyspec = pl.BlockSpec(memory_space=pl.ANY)
    return pl.pallas_call(
        functools.partial(gather_kernel, line, parts),
        out_shape=(
            jax.ShapeDtypeStruct((kinds, 2 * line * wrows, width), pieces.dtype),
            jax.ShapeDtypeStruct((2, 4 * toks.shape[0], toks.shape[1]), toks.dtype),
        ),
        in_specs=[anyspec] * 3,
        out_specs=(anyspec, anyspec),
        scratch_shapes=[
            pltpu.VMEM(pieces.shape[1:], pieces.dtype),
            pltpu.VMEM((2,) + toks.shape, toks.dtype),
            zsem, zsem, zsem, zsem,
            dma((parts,)), dma((parts,)),
            dma((6,)), dma((6,)), dma((6,)), dma((6,)),
            dma((3,)), dma((3,)),
        ],
        compiler_params=pltpu.CompilerParams(collective_id=0, has_side_effects=True),
        name="gather_all",
    )(pieces, toks, cots)


def reduce_kernel(
    line, p_in, g_in, gi_out, gd_out,
    r1, s1, rx, ry, s3, fin, u_in, d_in, u_out, d_out, gfin,
    c_s, c_r, x_s, x_r, yy_s, yy_r, u_s, u_r, d_s, d_r, f_s, f_r, o_s, o_r, loc,
):
    r = lax.axis_index("rep")
    f = lax.axis_index("fs")
    core = lax.axis_index("tp")
    z, y = f // 2, f % 2
    rows = p_in.shape[0] // 4
    cols = p_in.shape[1] // 2
    side = cols // 2
    width = g_in.shape[1]
    zrows = g_in.shape[0] // line
    frows = zrows // 2
    up = {"fs": (f + 2) % (2 * line)}
    dn = {"fs": (f + 2 * line - 2) % (2 * line)}
    ypart = {"fs": f + 1 - 2 * y}
    xpart = {"rep": 1 - r}
    cpart = {"tp": 1 - core}

    barrier = pltpu.get_barrier_semaphore()
    for dev in (ypart, xpart, cpart, up, dn):
        pl.semaphore_signal(barrier, inc=1, device_id=dev, device_id_type=MESH)
    pl.semaphore_wait(barrier, 5)

    def remote(src, dst, s, q, dev):
        return pltpu.make_async_remote_copy(
            src_ref=src, dst_ref=dst, send_sem=s, recv_sem=q,
            device_id=dev, device_id_type=MESH,
        )

    def total(dst, terms, count, step=64):
        @pl.loop(0, count // step)
        def _(i):
            at = pl.multiple_of(i * step, step)
            value = None
            for ref, row, col, wide in terms:
                one = ref[pl.ds(row + at, step), pl.ds(col, wide)].astype(jnp.float32)
                value = one if value is None else value + one
            ref, row, col, wide = dst
            ref[pl.ds(row + at, step), pl.ds(col, wide)] = value.astype(ref.dtype)

    def slot(rr, yy):
        return pl.multiple_of((2 * rr + yy) * rows, rows)

    order = [(1 - r, 1 - y), (1 - r, y), (r, 1 - y), (r, y)]
    my_col = pl.multiple_of(core * cols, cols)
    its_col = pl.multiple_of((1 - core) * cols, cols)

    def core_copy(i):
        at = pl.ds(slot(*order[i]), rows)
        return remote(p_in.at[at, pl.ds(its_col, cols)], r1.at[at, :], c_s.at[i], c_r.at[i], cpart)

    def s1_half(i, second):
        return s1.at[pl.ds(slot(*order[i]), rows), pl.ds(side if second else 0, side)]

    def x_copy(i):
        src = (s1_half(0, False), s1_half(1, False), s3.at[1])[i]
        return remote(src, rx.at[i], x_s.at[i], x_r.at[i], xpart)

    def y_copy(i):
        src = (s1_half(0, True), s1_half(2, True), s3.at[0])[i]
        return remote(src, ry.at[i], yy_s.at[i], yy_r.at[i], ypart)

    def block(ref, zt):
        return ref.at[pl.ds(zt * zrows, zrows), :]

    def up_copy(zt, first):
        return remote(block(g_in if first else u_out, zt), block(u_in, zt), u_s.at[zt], u_r.at[zt], up)

    def dn_copy(zt, first):
        return remote(block(g_in if first else d_out, zt), block(d_in, zt), d_s.at[zt], d_r.at[zt], dn)

    def line_step(i):
        zt = line - 1 - i
        if zt > 0:
            @pl.when((z > 0) & (z < zt))
            def _():
                up_copy(zt, False).wait_recv()
                row = zt * zrows
                total((u_out, row, 0, width), [(g_in, row, 0, width), (u_in, row, 0, width)], zrows)
                up_copy(zt, False).start()

            zd = i

            @pl.when((z < line - 1) & (z > zd))
            def _():
                dn_copy(zd, False).wait_recv()
                row = zd * zrows
                total((d_out, row, 0, width), [(g_in, row, 0, width), (d_in, row, 0, width)], zrows)
                dn_copy(zd, False).start()

    for i in range(4):
        core_copy(i).start()
    for i in range(line - 1):
        @pl.when(z == 0)
        def _():
            up_copy(line - 1 - i, True).start()

        @pl.when(z == line - 1)
        def _():
            dn_copy(i, True).start()

    for i in range(4):
        core_copy(i).wait_recv()
        row = slot(*order[i])
        total((s1, row, 0, cols), [(p_in, row, my_col, cols), (r1, row, 0, cols)], rows)
        if i in (0, 1):
            x_copy(i).start()
        if i == 0:
            y_copy(0).start()
        if i == 2:
            y_copy(1).start()

    line_step(0)
    x_copy(0).wait_recv()
    total((s3.at[0], 0, 0, side), [(s1, slot(r, 1 - y), 0, side), (rx.at[0], 0, 0, side)], rows)
    y_copy(2).start()
    y_copy(0).wait_recv()
    total((s3.at[1], 0, 0, side), [(s1, slot(1 - r, y), side, side), (ry.at[0], 0, 0, side)], rows)
    x_copy(2).start()
    for i in range(1, line - 1):
        line_step(i)

    zrow = pl.multiple_of(z * zrows, zrows)

    def here(ref):
        return (ref, zrow, 0, width)

    @pl.when(z == 0)
    def _():
        dn_copy(0, True).wait_recv()
        total((gfin, 0, 0, width), [here(g_in), here(d_in)], zrows)

    @pl.when(z == line - 1)
    def _():
        up_copy(line - 1, True).wait_recv()
        total((gfin, 0, 0, width), [here(g_in), here(u_in)], zrows)

    @pl.when((z > 0) & (z < line - 1))
    def _():
        remote(block(g_in, z), block(u_in, z), u_s.at[z], u_r.at[z], up).wait_recv()
        remote(block(g_in, z), block(d_in, z), d_s.at[z], d_r.at[z], dn).wait_recv()
        total((gfin, 0, 0, width), [here(g_in), here(u_in), here(d_in)], zrows)

    def gcols(rr, yy):
        return gd_out.at[:, pl.ds(pl.multiple_of((2 * rr + yy) * width, width), width)]

    def grows(yy):
        return gfin.at[pl.ds(pl.multiple_of(yy * frows, frows), frows), :]

    def f_copy(i, landing):
        if i == 0:
            dst = gcols(r, 1 - y) if landing else gcols(r, y)
            return remote(grows(1 - y), dst, f_s.at[0], f_r.at[0], ypart)
        if i == 1:
            dst = gcols(1 - r, y) if landing else gcols(r, y)
            return remote(grows(y), dst, f_s.at[1], f_r.at[1], xpart)
        dst = gcols(1 - r, 1 - y) if landing else gcols(r, 1 - y)
        return remote(gcols(r, 1 - y), dst, f_s.at[2], f_r.at[2], xpart)

    f_copy(0, False).start()
    f_copy(1, False).start()
    own_g = pltpu.make_async_copy(grows(y), gcols(r, y), loc.at[0])
    own_g.start()

    x_copy(1).wait_recv()
    y_copy(2).wait_recv()
    here_row = slot(r, y)
    total(
        (fin, 0, 0, side),
        [(s1, here_row, 0, side), (rx.at[1], 0, 0, side), (ry.at[2], 0, 0, side)], rows,
    )

    def o_copy(i, landing):
        base = (1 - core if landing else core) * cols + i * side
        dst = gi_out.at[:, pl.ds(pl.multiple_of(base, side), side)]
        return remote(fin.at[:, pl.ds(i * side, side)], dst, o_s.at[i], o_r.at[i], cpart)

    def o_local(i):
        base = pl.multiple_of(core * cols + i * side, side)
        return pltpu.make_async_copy(
            fin.at[:, pl.ds(i * side, side)], gi_out.at[:, pl.ds(base, side)], loc.at[1 + i]
        )

    o_copy(0, False).start()
    o_local(0).start()
    f_copy(0, True).wait_recv()
    f_copy(2, False).start()
    y_copy(1).wait_recv()
    x_copy(2).wait_recv()
    total(
        (fin, 0, side, side),
        [(s1, here_row, side, side), (ry.at[1], 0, 0, side), (rx.at[2], 0, 0, side)], rows,
    )
    o_copy(1, False).start()
    o_local(1).start()

    for i in range(4):
        core_copy(i).wait_send()
    for i in range(3):
        x_copy(i).wait_send()
        y_copy(i).wait_send()
        f_copy(i, False).wait_send()
    f_copy(1, True).wait_recv()
    f_copy(2, True).wait_recv()
    for i in range(2):
        o_copy(i, True).wait_recv()
        o_copy(i, False).wait_send()
        o_local(i).wait()
    own_g.wait()
    for zt in range(line):
        if zt > 0:
            pl.when(z < zt)(lambda: up_copy(zt, True).wait_send())
        if zt < line - 1:
            pl.when(z > zt)(lambda: dn_copy(zt, True).wait_send())


def reduced(part, grad_part):
    line = lax.axis_size("fs") // 2
    rows, cols = part.shape[0] // 4, part.shape[1] // 2
    depth, width = grad_part.shape
    kind = part.dtype
    dma = pltpu.SemaphoreType.DMA
    vmem = pl.BlockSpec(memory_space=pltpu.VMEM)
    anyspec = pl.BlockSpec(memory_space=pl.ANY)
    unit = pltpu.VMEM((3, rows, cols // 2), kind)
    whole = pltpu.VMEM((depth, width), kind)
    return pl.pallas_call(
        functools.partial(reduce_kernel, line),
        out_shape=(
            jax.ShapeDtypeStruct((rows, 2 * cols), kind),
            jax.ShapeDtypeStruct((depth // (2 * line), 4 * width), kind),
        ),
        in_specs=[vmem, vmem],
        out_specs=(anyspec, anyspec),
        scratch_shapes=[
            pltpu.VMEM((4 * rows, cols), kind),
            pltpu.VMEM((4 * rows, cols), kind),
            unit, unit,
            pltpu.VMEM((2, rows, cols // 2), kind),
            pltpu.VMEM((rows, cols), kind),
            whole, whole, whole, whole,
            pltpu.VMEM((depth // line, width), kind),
            dma((4,)), dma((4,)), dma((3,)), dma((3,)), dma((3,)), dma((3,)),
            dma((line,)), dma((line,)), dma((line,)), dma((line,)),
            dma((3,)), dma((3,)), dma((2,)), dma((2,)), dma((3,)),
        ],
        compiler_params=pltpu.CompilerParams(
            collective_id=1, has_side_effects=True, vmem_limit_bytes=56 * 2**20
        ),
        name="reduce_all",
    )(part, grad_part)


def on_device(inputs, cotangent, gate_weight, up_weight, down_weight):
    tok_rows = inputs.shape[0]
    fs_size = lax.axis_size("fs")
    rep_size = lax.axis_size("rep")
    contract = (((1,), (1,)), ((), ()))
    contract_tok = (((0,), (0,)), ((), ()))
    width = gate_weight.shape[1] // 4
    r = lax.axis_index("rep")
    y = lax.axis_index("fs") % 2

    def piece(side):
        return jnp.stack([
            lax.dynamic_slice_in_dim(weight, (2 * r + side) * width, width, 1)
            for weight in (gate_weight, up_weight, down_weight)
        ])

    weights, tokens = gather(jnp.stack([piece(0), piece(1)]), inputs, cotangent)
    gate_full, up_full, down_full = weights[0], weights[1], weights[2]
    gate_val = jnp.dot(tokens[0], gate_full, preferred_element_type=jnp.float32)
    up_val = jnp.dot(tokens[0], up_full, preferred_element_type=jnp.float32)
    grad_hidden = jnp.dot(tokens[1], down_full, preferred_element_type=jnp.float32)
    sigmoid_gate = jax.nn.sigmoid(gate_val)
    active = gate_val * sigmoid_gate
    hidden = (active * up_val).astype(jnp.bfloat16)
    grad_gate = (
        grad_hidden * up_val * sigmoid_gate * (1.0 + gate_val * (1.0 - sigmoid_gate))
    ).astype(jnp.bfloat16)
    grad_up = (grad_hidden * active).astype(jnp.bfloat16)
    grad_scale = 1.0 / math.sqrt(tok_rows * fs_size * rep_size)
    pairs = [[i, i + 1] for i in range(0, fs_size, 2)]
    lines = [list(range(i, fs_size, 2)) for i in range(2)]
    grad_part = lax.dot_general(
        tokens[1], hidden, contract_tok, preferred_element_type=jnp.float32
    )
    part = lax.dot_general(
        grad_gate, gate_full, contract, preferred_element_type=jnp.float32
    )
    part = part + lax.dot_general(
        grad_up, up_full, contract, preferred_element_type=jnp.float32
    )
    if lax.axis_size("tp") == 2:
        grad_input, grad_down = reduced(
            part.astype(jnp.bfloat16), grad_part.astype(jnp.bfloat16)
        )
        return (grad_input, grad_down.astype(jnp.float32) * grad_scale)
    shard = lax.psum_scatter(
        grad_part.astype(jnp.bfloat16), "fs", scatter_dimension=0, tiled=True,
        axis_index_groups=lines,
    ).astype(jnp.float32) * grad_scale
    shard = lax.all_to_all(
        shard, "fs", split_axis=0, concat_axis=1, tiled=True, axis_index_groups=pairs
    )
    grad_down = lax.all_gather(shard, "rep", axis=1, tiled=True)
    part = lax.psum_scatter(
        part.astype(jnp.bfloat16), "rep", scatter_dimension=0, tiled=True
    )
    part = lax.psum_scatter(
        part, "fs", scatter_dimension=0, tiled=True, axis_index_groups=pairs
    )
    grad_input = lax.psum(part, "tp")
    return (grad_input, grad_down)


def solution(mesh):
    placed = (
        P(("rep", "fs"), None),
        P(("rep", "fs"), None),
        P("fs", "tp"),
        P("fs", "tp"),
        P("fs", "tp"),
    )
    return jax.shard_map(
        on_device,
        mesh=mesh,
        in_specs=placed,
        out_specs=(P(("rep", "fs"), None), P("fs", "tp")),
        check_vma=False,
    )
```

```python
import functools
import math

import jax
import jax.numpy as jnp
from jax import lax
from jax.experimental import pallas as pl
from jax.experimental.pallas import tpu as pltpu
from jax.sharding import PartitionSpec as P

MESH = pl.DeviceIdType.MESH


def gather_kernel(
    line, units, gu_pieces, d_pieces, toks, cots, gu_out, d_out, t_out, gu_tmp, d_tmp, t_tmp,
    up_s, up_r, dn_s, dn_r, y_s, y_r, tok_s, tok_r, d2d_s, d2d_r, loc, loc2,
):
    r = lax.axis_index("rep")
    f = lax.axis_index("fs")
    t = lax.axis_index("tp")
    z, y = f // 2, f % 2
    rows = toks.shape[0]
    half = rows // 2
    wrows = gu_pieces.shape[1]
    parts = len(units)
    has_up, has_dn = z < line - 1, z > 0
    up = {"fs": (f + 2) % (2 * line)}
    dn = {"fs": (f + 2 * line - 2) % (2 * line)}
    ypart = {"fs": f + 1 - 2 * y}
    xpart = {"rep": 1 - r}
    core = t % 2
    cpart = {"tp": t + 1 - 2 * core}

    barrier = pltpu.get_barrier_semaphore()

    def greet(dev):
        pl.semaphore_signal(barrier, inc=1, device_id=dev, device_id_type=MESH)

    for dev in (ypart, xpart, cpart, up, dn):
        greet(dev)
    pl.semaphore_wait(barrier, 5)

    def remote(src, dst, s, q, dev):
        return pltpu.make_async_remote_copy(
            src_ref=src, dst_ref=dst, send_sem=s, recv_sem=q,
            device_id=dev, device_id_type=MESH,
        )

    def wblk(k, zz, yy):
        row = pl.multiple_of((2 * zz + yy) * wrows, wrows)
        which, col, wide = units[k]
        return (gu_out, d_out)[which].at[pl.ds(row, wrows), pl.ds(col, wide)]

    def own(k, yy):
        which, col, wide = units[k]
        return (gu_pieces, d_pieces)[which].at[yy, :, pl.ds(col, wide)]

    def to_y(k):
        return remote(own(k, 1 - y), wblk(k, z, y), y_s.at[k], y_r.at[k], ypart)

    def from_y(k):
        return remote(own(k, 1 - y), wblk(k, z, 1 - y), y_s.at[k], y_r.at[k], ypart)

    def zcopy(up_dir, d, sub, k, zz):
        yy = y if sub == 0 else 1 - y
        src = own(k, y) if (d == 0 and sub == 0) else wblk(k, zz, yy)
        s, q, dev = (up_s, up_r, up) if up_dir else (dn_s, dn_r, dn)
        return remote(src, wblk(k, zz, yy), s.at[d, sub, k], q.at[d, sub, k], dev)

    def pred_send(up_dir, d):
        return (has_up & (z - d >= 0)) if up_dir else (has_dn & (z + d <= line - 1))

    def src_z(up_dir, d):
        return jnp.maximum(z - d, 0) if up_dir else jnp.minimum(z + d, line - 1)

    def send(up_dir, d, sub, k):
        @pl.when(pred_send(up_dir, d))
        def _():
            zcopy(up_dir, d, sub, k, src_z(up_dir, d)).start()

    def await_send(up_dir, d, sub, k):
        @pl.when(pred_send(up_dir, d))
        def _():
            zcopy(up_dir, d, sub, k, src_z(up_dir, d)).wait_send()

    def await_recv(up_dir, d, sub, k):
        ok = (z - d - 1 >= 0) if up_dir else (z + d + 1 <= line - 1)

        @pl.when(ok)
        def _():
            zcopy(up_dir, d, sub, k, src_z(up_dir, d + 1)).wait_recv()

    def tblk(j, rr, yy, c):
        row = pl.multiple_of((2 * rr + yy) * rows + c * half, half)
        return t_out.at[j, pl.ds(row, half), :]

    def mine(j):
        src = toks if j == 0 else cots
        return src.at[pl.ds(pl.multiple_of(core * half, half), half), :]

    def tcopy(i, landing):
        j = (0, 1, 0, 1, 0, 1)[i]
        dev = xpart if i in (0, 1, 5) else ypart
        if landing:
            rr = (1 - r, 1 - r, r, r, 1 - r, 1 - r)[i]
            yy = (y, y, 1 - y, 1 - y, 1 - y, 1 - y)[i]
            src = dst = tblk(j, rr, yy, core)
        else:
            rr = (r, r, r, r, 1 - r, r)[i]
            yy = (y, y, y, y, y, 1 - y)[i]
            dst = tblk(j, rr, yy, core)
            src = mine(j) if i < 4 else dst
        return remote(src, dst, tok_s.at[i], tok_r.at[i], dev)

    def dcopy(i, c):
        j = (0, 1, 0, 1, 0, 1)[i]
        rr = (1 - r, 1 - r, r, r, 1 - r, 1 - r)[i]
        yy = (y, y, 1 - y, 1 - y, 1 - y, 1 - y)[i]
        blk = tblk(j, rr, yy, c)
        return remote(blk, blk, d2d_s.at[i], d2d_r.at[i], cpart)

    loads = [
        pltpu.make_async_copy(gu_pieces.at[y], gu_tmp, loc.at[0]),
        pltpu.make_async_copy(d_pieces.at[y], d_tmp, loc.at[3]),
        pltpu.make_async_copy(toks, t_tmp.at[0], loc.at[1]),
        pltpu.make_async_copy(cots, t_tmp.at[1], loc.at[2]),
    ]
    trow = pl.multiple_of((2 * r + y) * rows, rows)
    wrow = pl.multiple_of(f * wrows, wrows)
    stores = [
        pltpu.make_async_copy(gu_tmp, gu_out.at[pl.ds(wrow, wrows), :], loc2.at[0]),
        pltpu.make_async_copy(d_tmp, d_out.at[pl.ds(wrow, wrows), :], loc2.at[3]),
        pltpu.make_async_copy(t_tmp.at[0], t_out.at[0, pl.ds(trow, rows), :], loc2.at[1]),
        pltpu.make_async_copy(t_tmp.at[1], t_out.at[1, pl.ds(trow, rows), :], loc2.at[2]),
    ]

    for k in range(parts):
        to_y(k).start()
        send(True, 0, 0, k)
        send(False, 0, 0, k)
    for i in (0, 1, 3, 2):
        tcopy(i, False).start()
    for copy in loads:
        copy.start()
    for load, store in zip(loads, stores):
        load.wait()
        store.start()
    for k in range(parts):
        from_y(k).wait_recv()
        send(True, 0, 1, k)
        send(False, 0, 1, k)

    def event(i):
        tcopy(i, True).wait_recv()
        if i == 0:
            tcopy(4, False).start()
        if i == 3:
            tcopy(5, False).start()
        dcopy(i, core).start()

    events = [0, 3, 1, 2, 5, 4]
    for d in range(line - 1):
        for sub in range(2):
            if events:
                event(events.pop(0))
            for k in range(parts):
                for up_dir in (True, False):
                    await_recv(up_dir, d, sub, k)
                    if d + 1 < line - 1:
                        send(up_dir, d + 1, sub, k)
    for i in events:
        event(i)
    for i in range(6):
        dcopy(i, 1 - core).wait_recv()
        dcopy(i, core).wait_send()
        tcopy(i, False).wait_send()
    for k in range(parts):
        to_y(k).wait_send()
        for d in range(line - 1):
            for sub in range(2):
                await_send(True, d, sub, k)
                await_send(False, d, sub, k)
    for store in stores:
        store.wait()


def gather(gu_pieces, d_pieces, toks, cots):
    line = lax.axis_size("fs") // 2
    _, wrows, width = d_pieces.shape
    units = [(0, 0, 2 * width), (1, 0, width)]
    if line <= 4:
        units = [(0, 0, width), (0, width, width), (1, 0, width)]
    parts = len(units)
    depth = 2 * line * wrows
    kind = d_pieces.dtype
    dma = pltpu.SemaphoreType.DMA
    zsem = dma((line - 1, 2, parts))
    anyspec = pl.BlockSpec(memory_space=pl.ANY)
    return pl.pallas_call(
        functools.partial(gather_kernel, line, units),
        out_shape=(
            jax.ShapeDtypeStruct((depth, 2 * width), kind),
            jax.ShapeDtypeStruct((depth, width), kind),
            jax.ShapeDtypeStruct((2, 4 * toks.shape[0], toks.shape[1]), toks.dtype),
        ),
        in_specs=[anyspec] * 4,
        out_specs=(anyspec,) * 3,
        scratch_shapes=[
            pltpu.VMEM(gu_pieces.shape[1:], kind),
            pltpu.VMEM(d_pieces.shape[1:], kind),
            pltpu.VMEM((2,) + toks.shape, toks.dtype),
            zsem, zsem, zsem, zsem,
            dma((parts,)), dma((parts,)),
            dma((6,)), dma((6,)), dma((6,)), dma((6,)),
            dma((4,)), dma((4,)),
        ],
        compiler_params=pltpu.CompilerParams(collective_id=0, has_side_effects=True),
        name="gather_all",
    )(gu_pieces, d_pieces, toks, cots)


def reduce_kernel(
    line, p_in, g_in, gi_out, gd_out,
    r1, s1, rx, ry, s3, fin, u_in, d_in, u_out, d_out, gfin,
    c_s, c_r, x_s, x_r, yy_s, yy_r, u_s, u_r, d_s, d_r, f_s, f_r, o_s, o_r, loc,
):
    r = lax.axis_index("rep")
    f = lax.axis_index("fs")
    core = lax.axis_index("tp")
    z, y = f // 2, f % 2
    rows = p_in.shape[0] // 4
    cols = p_in.shape[1] // 2
    side = cols // 2
    width = g_in.shape[1]
    zrows = g_in.shape[0] // line
    frows = zrows // 2
    up = {"fs": (f + 2) % (2 * line)}
    dn = {"fs": (f + 2 * line - 2) % (2 * line)}
    ypart = {"fs": f + 1 - 2 * y}
    xpart = {"rep": 1 - r}
    cpart = {"tp": 1 - core}

    barrier = pltpu.get_barrier_semaphore()
    for dev in (ypart, xpart, cpart, up, dn):
        pl.semaphore_signal(barrier, inc=1, device_id=dev, device_id_type=MESH)
    pl.semaphore_wait(barrier, 5)

    def remote(src, dst, s, q, dev):
        return pltpu.make_async_remote_copy(
            src_ref=src, dst_ref=dst, send_sem=s, recv_sem=q,
            device_id=dev, device_id_type=MESH,
        )

    def total(dst, terms, count, step=64):
        @pl.loop(0, count // step)
        def _(i):
            at = pl.multiple_of(i * step, step)
            value = None
            for ref, row, col, wide in terms:
                one = ref[pl.ds(row + at, step), pl.ds(col, wide)].astype(jnp.float32)
                value = one if value is None else value + one
            ref, row, col, wide = dst
            ref[pl.ds(row + at, step), pl.ds(col, wide)] = value.astype(ref.dtype)

    def slot(rr, yy):
        return pl.multiple_of((2 * rr + yy) * rows, rows)

    order = [(1 - r, 1 - y), (1 - r, y), (r, 1 - y), (r, y)]
    my_col = pl.multiple_of(core * cols, cols)
    its_col = pl.multiple_of((1 - core) * cols, cols)

    def core_copy(i):
        at = pl.ds(slot(*order[i]), rows)
        return remote(p_in.at[at, pl.ds(its_col, cols)], r1.at[at, :], c_s.at[i], c_r.at[i], cpart)

    def s1_half(i, second):
        return s1.at[pl.ds(slot(*order[i]), rows), pl.ds(side if second else 0, side)]

    def x_copy(i):
        src = (s1_half(0, False), s1_half(1, False), s3.at[1])[i]
        return remote(src, rx.at[i], x_s.at[i], x_r.at[i], xpart)

    def y_copy(i):
        src = (s1_half(0, True), s1_half(2, True), s3.at[0])[i]
        return remote(src, ry.at[i], yy_s.at[i], yy_r.at[i], ypart)

    def block(ref, zt):
        return ref.at[pl.ds(zt * zrows, zrows), :]

    def up_copy(zt, first):
        return remote(block(g_in if first else u_out, zt), block(u_in, zt), u_s.at[zt], u_r.at[zt], up)

    def dn_copy(zt, first):
        return remote(block(g_in if first else d_out, zt), block(d_in, zt), d_s.at[zt], d_r.at[zt], dn)

    def line_step(i):
        zt = line - 1 - i
        if zt > 0:
            @pl.when((z > 0) & (z < zt))
            def _():
                up_copy(zt, False).wait_recv()
                row = zt * zrows
                total((u_out, row, 0, width), [(g_in, row, 0, width), (u_in, row, 0, width)], zrows)
                up_copy(zt, False).start()

            zd = i

            @pl.when((z < line - 1) & (z > zd))
            def _():
                dn_copy(zd, False).wait_recv()
                row = zd * zrows
                total((d_out, row, 0, width), [(g_in, row, 0, width), (d_in, row, 0, width)], zrows)
                dn_copy(zd, False).start()

    for i in range(4):
        core_copy(i).start()
    for i in range(line - 1):
        @pl.when(z == 0)
        def _():
            up_copy(line - 1 - i, True).start()

        @pl.when(z == line - 1)
        def _():
            dn_copy(i, True).start()

    for i in range(4):
        core_copy(i).wait_recv()
        row = slot(*order[i])
        total((s1, row, 0, cols), [(p_in, row, my_col, cols), (r1, row, 0, cols)], rows)
        if i in (0, 1):
            x_copy(i).start()
        if i == 0:
            y_copy(0).start()
        if i == 2:
            y_copy(1).start()

    line_step(0)
    x_copy(0).wait_recv()
    total((s3.at[0], 0, 0, side), [(s1, slot(r, 1 - y), 0, side), (rx.at[0], 0, 0, side)], rows)
    y_copy(2).start()
    y_copy(0).wait_recv()
    total((s3.at[1], 0, 0, side), [(s1, slot(1 - r, y), side, side), (ry.at[0], 0, 0, side)], rows)
    x_copy(2).start()
    for i in range(1, line - 1):
        line_step(i)

    zrow = pl.multiple_of(z * zrows, zrows)

    def here(ref):
        return (ref, zrow, 0, width)

    @pl.when(z == 0)
    def _():
        dn_copy(0, True).wait_recv()
        total((gfin, 0, 0, width), [here(g_in), here(d_in)], zrows)

    @pl.when(z == line - 1)
    def _():
        up_copy(line - 1, True).wait_recv()
        total((gfin, 0, 0, width), [here(g_in), here(u_in)], zrows)

    @pl.when((z > 0) & (z < line - 1))
    def _():
        remote(block(g_in, z), block(u_in, z), u_s.at[z], u_r.at[z], up).wait_recv()
        remote(block(g_in, z), block(d_in, z), d_s.at[z], d_r.at[z], dn).wait_recv()
        total((gfin, 0, 0, width), [here(g_in), here(u_in), here(d_in)], zrows)

    def gcols(rr, yy):
        return gd_out.at[:, pl.ds(pl.multiple_of((2 * rr + yy) * width, width), width)]

    def grows(yy):
        return gfin.at[pl.ds(pl.multiple_of(yy * frows, frows), frows), :]

    def f_copy(i, landing):
        if i == 0:
            dst = gcols(r, 1 - y) if landing else gcols(r, y)
            return remote(grows(1 - y), dst, f_s.at[0], f_r.at[0], ypart)
        if i == 1:
            dst = gcols(1 - r, y) if landing else gcols(r, y)
            return remote(grows(y), dst, f_s.at[1], f_r.at[1], xpart)
        dst = gcols(1 - r, 1 - y) if landing else gcols(r, 1 - y)
        return remote(gcols(r, 1 - y), dst, f_s.at[2], f_r.at[2], xpart)

    f_copy(0, False).start()
    f_copy(1, False).start()
    own_g = pltpu.make_async_copy(grows(y), gcols(r, y), loc.at[0])
    own_g.start()

    x_copy(1).wait_recv()
    y_copy(2).wait_recv()
    here_row = slot(r, y)
    total(
        (fin, 0, 0, side),
        [(s1, here_row, 0, side), (rx.at[1], 0, 0, side), (ry.at[2], 0, 0, side)], rows,
    )

    def o_copy(i, landing):
        base = (1 - core if landing else core) * cols + i * side
        dst = gi_out.at[:, pl.ds(pl.multiple_of(base, side), side)]
        return remote(fin.at[:, pl.ds(i * side, side)], dst, o_s.at[i], o_r.at[i], cpart)

    def o_local(i):
        base = pl.multiple_of(core * cols + i * side, side)
        return pltpu.make_async_copy(
            fin.at[:, pl.ds(i * side, side)], gi_out.at[:, pl.ds(base, side)], loc.at[1 + i]
        )

    o_copy(0, False).start()
    o_local(0).start()
    f_copy(0, True).wait_recv()
    f_copy(2, False).start()
    y_copy(1).wait_recv()
    x_copy(2).wait_recv()
    total(
        (fin, 0, side, side),
        [(s1, here_row, side, side), (ry.at[1], 0, 0, side), (rx.at[2], 0, 0, side)], rows,
    )
    o_copy(1, False).start()
    o_local(1).start()

    for i in range(4):
        core_copy(i).wait_send()
    for i in range(3):
        x_copy(i).wait_send()
        y_copy(i).wait_send()
        f_copy(i, False).wait_send()
    f_copy(1, True).wait_recv()
    f_copy(2, True).wait_recv()
    for i in range(2):
        o_copy(i, True).wait_recv()
        o_copy(i, False).wait_send()
        o_local(i).wait()
    own_g.wait()
    for zt in range(line):
        if zt > 0:
            pl.when(z < zt)(lambda: up_copy(zt, True).wait_send())
        if zt < line - 1:
            pl.when(z > zt)(lambda: dn_copy(zt, True).wait_send())


def reduced(part, grad_part):
    line = lax.axis_size("fs") // 2
    rows, cols = part.shape[0] // 4, part.shape[1] // 2
    depth, width = grad_part.shape
    kind = part.dtype
    dma = pltpu.SemaphoreType.DMA
    vmem = pl.BlockSpec(memory_space=pltpu.VMEM)
    anyspec = pl.BlockSpec(memory_space=pl.ANY)
    unit = pltpu.VMEM((3, rows, cols // 2), kind)
    whole = pltpu.VMEM((depth, width), kind)
    return pl.pallas_call(
        functools.partial(reduce_kernel, line),
        out_shape=(
            jax.ShapeDtypeStruct((rows, 2 * cols), kind),
            jax.ShapeDtypeStruct((depth // (2 * line), 4 * width), kind),
        ),
        in_specs=[vmem, vmem],
        out_specs=(anyspec, anyspec),
        scratch_shapes=[
            pltpu.VMEM((4 * rows, cols), kind),
            pltpu.VMEM((4 * rows, cols), kind),
            unit, unit,
            pltpu.VMEM((2, rows, cols // 2), kind),
            pltpu.VMEM((rows, cols), kind),
            whole, whole, whole, whole,
            pltpu.VMEM((depth // line, width), kind),
            dma((4,)), dma((4,)), dma((3,)), dma((3,)), dma((3,)), dma((3,)),
            dma((line,)), dma((line,)), dma((line,)), dma((line,)),
            dma((3,)), dma((3,)), dma((2,)), dma((2,)), dma((3,)),
        ],
        compiler_params=pltpu.CompilerParams(
            collective_id=1, has_side_effects=True, vmem_limit_bytes=56 * 2**20
        ),
        name="reduce_all",
    )(part, grad_part)


def on_device(inputs, cotangent, gate_weight, up_weight, down_weight):
    tok_rows = inputs.shape[0]
    fs_size = lax.axis_size("fs")
    rep_size = lax.axis_size("rep")
    contract = (((1,), (1,)), ((), ()))
    contract_tok = (((0,), (0,)), ((), ()))
    width = gate_weight.shape[1] // 4
    r = lax.axis_index("rep")
    y = lax.axis_index("fs") % 2

    def piece(weight, side):
        return lax.dynamic_slice_in_dim(weight, (2 * r + side) * width, width, 1)

    def both(side):
        return jnp.concatenate([piece(gate_weight, side), piece(up_weight, side)], axis=1)

    gate_up, down_full, tokens = gather(
        jnp.stack([both(0), both(1)]),
        jnp.stack([piece(down_weight, 0), piece(down_weight, 1)]),
        inputs,
        cotangent,
    )
    gate_up_val = jnp.dot(tokens[0], gate_up, preferred_element_type=jnp.float32)
    gate_val, up_val = gate_up_val[:, :width], gate_up_val[:, width:]
    grad_hidden = jnp.dot(tokens[1], down_full, preferred_element_type=jnp.float32)
    sigmoid_gate = jax.nn.sigmoid(gate_val)
    active = gate_val * sigmoid_gate
    hidden = (active * up_val).astype(jnp.bfloat16)
    grad_gate = (
        grad_hidden * up_val * sigmoid_gate * (1.0 + gate_val * (1.0 - sigmoid_gate))
    ).astype(jnp.bfloat16)
    grad_up = (grad_hidden * active).astype(jnp.bfloat16)
    grad_scale = 1.0 / math.sqrt(tok_rows * fs_size * rep_size)
    pairs = [[i, i + 1] for i in range(0, fs_size, 2)]
    lines = [list(range(i, fs_size, 2)) for i in range(2)]
    grad_part = lax.dot_general(
        tokens[1], hidden, contract_tok, preferred_element_type=jnp.float32
    )
    part = lax.dot_general(
        jnp.concatenate([grad_gate, grad_up], axis=1), gate_up, contract,
        preferred_element_type=jnp.float32,
    )
    if lax.axis_size("tp") == 2:
        grad_input, grad_down = reduced(
            part.astype(jnp.bfloat16), grad_part.astype(jnp.bfloat16)
        )
        return (grad_input, grad_down.astype(jnp.float32) * grad_scale)
    shard = lax.psum_scatter(
        grad_part.astype(jnp.bfloat16), "fs", scatter_dimension=0, tiled=True,
        axis_index_groups=lines,
    ).astype(jnp.float32) * grad_scale
    shard = lax.all_to_all(
        shard, "fs", split_axis=0, concat_axis=1, tiled=True, axis_index_groups=pairs
    )
    grad_down = lax.all_gather(shard, "rep", axis=1, tiled=True)
    part = lax.psum_scatter(
        part.astype(jnp.bfloat16), "rep", scatter_dimension=0, tiled=True
    )
    part = lax.psum_scatter(
        part, "fs", scatter_dimension=0, tiled=True, axis_index_groups=pairs
    )
    grad_input = lax.psum(part, "tp")
    return (grad_input, grad_down)


def solution(mesh):
    placed = (
        P(("rep", "fs"), None),
        P(("rep", "fs"), None),
        P("fs", "tp"),
        P("fs", "tp"),
        P("fs", "tp"),
    )
    return jax.shard_map(
        on_device,
        mesh=mesh,
        in_specs=placed,
        out_specs=(P(("rep", "fs"), None), P("fs", "tp")),
        check_vma=False,
    )
```

```python
import functools
import math

import jax
import jax.numpy as jnp
from jax import lax
from jax.experimental import pallas as pl
from jax.experimental.pallas import tpu as pltpu
from jax.sharding import PartitionSpec as P

MESH = pl.DeviceIdType.MESH


def gather_kernel(
    line, units, gate_w, up_w, down_w, toks, cots, gu_out, d_out, t_out, w_tmp, t_tmp,
    up_s, up_r, dn_s, dn_r, y_s, y_r, tok_s, tok_r, d2d_s, d2d_r, loc, loc2,
):
    r = lax.axis_index("rep")
    f = lax.axis_index("fs")
    t = lax.axis_index("tp")
    z, y = f // 2, f % 2
    rows = toks.shape[0]
    half = rows // 2
    wrows = gate_w.shape[0]
    width = gate_w.shape[1] // 4
    parts = len(units)
    has_up, has_dn = z < line - 1, z > 0
    up = {"fs": (f + 2) % (2 * line)}
    dn = {"fs": (f + 2 * line - 2) % (2 * line)}
    ypart = {"fs": f + 1 - 2 * y}
    xpart = {"rep": 1 - r}
    core = t % 2
    cpart = {"tp": t + 1 - 2 * core}

    barrier = pltpu.get_barrier_semaphore()

    def greet(dev):
        pl.semaphore_signal(barrier, inc=1, device_id=dev, device_id_type=MESH)

    for dev in (ypart, xpart, cpart, up, dn):
        greet(dev)
    pl.semaphore_wait(barrier, 5)

    def remote(src, dst, s, q, dev):
        return pltpu.make_async_remote_copy(
            src_ref=src, dst_ref=dst, send_sem=s, recv_sem=q,
            device_id=dev, device_id_type=MESH,
        )

    def wblk(k, zz, yy):
        row = pl.multiple_of((2 * zz + yy) * wrows, wrows)
        which, col, wide = units[k]
        return (gu_out, d_out)[which].at[pl.ds(row, wrows), pl.ds(col, wide)]

    def own(k, yy):
        col = pl.multiple_of((2 * r + yy) * width, width)
        return (gate_w, up_w, down_w)[k].at[:, pl.ds(col, width)]

    def to_y(k):
        return remote(own(k, 1 - y), wblk(k, z, y), y_s.at[k], y_r.at[k], ypart)

    def from_y(k):
        return remote(own(k, 1 - y), wblk(k, z, 1 - y), y_s.at[k], y_r.at[k], ypart)

    def zcopy(up_dir, d, sub, k, zz):
        yy = y if sub == 0 else 1 - y
        src = own(k, y) if (d == 0 and sub == 0) else wblk(k, zz, yy)
        s, q, dev = (up_s, up_r, up) if up_dir else (dn_s, dn_r, dn)
        return remote(src, wblk(k, zz, yy), s.at[d, sub, k], q.at[d, sub, k], dev)

    def pred_send(up_dir, d):
        return (has_up & (z - d >= 0)) if up_dir else (has_dn & (z + d <= line - 1))

    def src_z(up_dir, d):
        return jnp.maximum(z - d, 0) if up_dir else jnp.minimum(z + d, line - 1)

    def send(up_dir, d, sub, k):
        @pl.when(pred_send(up_dir, d))
        def _():
            zcopy(up_dir, d, sub, k, src_z(up_dir, d)).start()

    def await_send(up_dir, d, sub, k):
        @pl.when(pred_send(up_dir, d))
        def _():
            zcopy(up_dir, d, sub, k, src_z(up_dir, d)).wait_send()

    def await_recv(up_dir, d, sub, k):
        ok = (z - d - 1 >= 0) if up_dir else (z + d + 1 <= line - 1)

        @pl.when(ok)
        def _():
            zcopy(up_dir, d, sub, k, src_z(up_dir, d + 1)).wait_recv()

    def tblk(j, rr, yy, c):
        row = pl.multiple_of((2 * rr + yy) * rows + c * half, half)
        return t_out.at[j, pl.ds(row, half), :]

    def mine(j):
        src = toks if j == 0 else cots
        return src.at[pl.ds(pl.multiple_of(core * half, half), half), :]

    def tcopy(i, landing):
        j = (0, 1, 0, 1, 0, 1)[i]
        dev = xpart if i in (0, 1, 5) else ypart
        if landing:
            rr = (1 - r, 1 - r, r, r, 1 - r, 1 - r)[i]
            yy = (y, y, 1 - y, 1 - y, 1 - y, 1 - y)[i]
            src = dst = tblk(j, rr, yy, core)
        else:
            rr = (r, r, r, r, 1 - r, r)[i]
            yy = (y, y, y, y, y, 1 - y)[i]
            dst = tblk(j, rr, yy, core)
            src = mine(j) if i < 4 else dst
        return remote(src, dst, tok_s.at[i], tok_r.at[i], dev)

    def dcopy(i, c):
        j = (0, 1, 0, 1, 0, 1)[i]
        rr = (1 - r, 1 - r, r, r, 1 - r, 1 - r)[i]
        yy = (y, y, 1 - y, 1 - y, 1 - y, 1 - y)[i]
        blk = tblk(j, rr, yy, c)
        return remote(blk, blk, d2d_s.at[i], d2d_r.at[i], cpart)

    loads = [
        pltpu.make_async_copy(own(0, y), w_tmp.at[0], loc.at[0]),
        pltpu.make_async_copy(own(1, y), w_tmp.at[1], loc.at[3]),
        pltpu.make_async_copy(own(2, y), w_tmp.at[2], loc.at[4]),
        pltpu.make_async_copy(toks, t_tmp.at[0], loc.at[1]),
        pltpu.make_async_copy(cots, t_tmp.at[1], loc.at[2]),
    ]
    trow = pl.multiple_of((2 * r + y) * rows, rows)
    stores = [
        pltpu.make_async_copy(w_tmp.at[0], wblk(0, z, y), loc2.at[0]),
        pltpu.make_async_copy(w_tmp.at[1], wblk(1, z, y), loc2.at[3]),
        pltpu.make_async_copy(w_tmp.at[2], wblk(2, z, y), loc2.at[4]),
        pltpu.make_async_copy(t_tmp.at[0], t_out.at[0, pl.ds(trow, rows), :], loc2.at[1]),
        pltpu.make_async_copy(t_tmp.at[1], t_out.at[1, pl.ds(trow, rows), :], loc2.at[2]),
    ]

    for k in range(parts):
        to_y(k).start()
        send(True, 0, 0, k)
        send(False, 0, 0, k)
    for i in (0, 1, 3, 2):
        tcopy(i, False).start()
    for copy in loads:
        copy.start()
    for load, store in zip(loads, stores):
        load.wait()
        store.start()
    for k in range(parts):
        from_y(k).wait_recv()
        send(True, 0, 1, k)
        send(False, 0, 1, k)

    def event(i):
        tcopy(i, True).wait_recv()
        if i == 0:
            tcopy(4, False).start()
        if i == 3:
            tcopy(5, False).start()
        dcopy(i, core).start()

    events = [0, 3, 1, 2, 5, 4]
    for d in range(line - 1):
        for sub in range(2):
            if events:
                event(events.pop(0))
            for k in range(parts):
                for up_dir in (True, False):
                    await_recv(up_dir, d, sub, k)
                    if d + 1 < line - 1:
                        send(up_dir, d + 1, sub, k)
    for i in events:
        event(i)
    for i in range(6):
        dcopy(i, 1 - core).wait_recv()
        dcopy(i, core).wait_send()
        tcopy(i, False).wait_send()
    for k in range(parts):
        to_y(k).wait_send()
        for d in range(line - 1):
            for sub in range(2):
                await_send(True, d, sub, k)
                await_send(False, d, sub, k)
    for store in stores:
        store.wait()


def gather(gate_w, up_w, down_w, toks, cots):
    line = lax.axis_size("fs") // 2
    wrows, width = gate_w.shape[0], gate_w.shape[1] // 4
    units = [(0, 0, width), (0, width, width), (1, 0, width)]
    parts = len(units)
    depth = 2 * line * wrows
    kind = gate_w.dtype
    dma = pltpu.SemaphoreType.DMA
    zsem = dma((line - 1, 2, parts))
    anyspec = pl.BlockSpec(memory_space=pl.ANY)
    return pl.pallas_call(
        functools.partial(gather_kernel, line, units),
        out_shape=(
            jax.ShapeDtypeStruct((depth, 2 * width), kind),
            jax.ShapeDtypeStruct((depth, width), kind),
            jax.ShapeDtypeStruct((2, 4 * toks.shape[0], toks.shape[1]), toks.dtype),
        ),
        in_specs=[anyspec] * 5,
        out_specs=(anyspec,) * 3,
        scratch_shapes=[
            pltpu.VMEM((parts, wrows, width), kind),
            pltpu.VMEM((2,) + toks.shape, toks.dtype),
            zsem, zsem, zsem, zsem,
            dma((parts,)), dma((parts,)),
            dma((6,)), dma((6,)), dma((6,)), dma((6,)),
            dma((5,)), dma((5,)),
        ],
        compiler_params=pltpu.CompilerParams(collective_id=0, has_side_effects=True),
        name="gather_all",
    )(gate_w, up_w, down_w, toks, cots)


def reduce_kernel(
    line, p_in, g_in, gi_out, gd_out,
    p_tmp, r1, s1, rx, ry, s3, fin, u_in, d_in, u_out, d_out, gfin,
    c_s, c_r, x_s, x_r, yy_s, yy_r, u_s, u_r, d_s, d_r, f_s, f_r, o_s, o_r, loc,
):
    r = lax.axis_index("rep")
    f = lax.axis_index("fs")
    core = lax.axis_index("tp")
    z, y = f // 2, f % 2
    rows = p_in.shape[0] // 4
    cols = p_in.shape[1] // 2
    side = cols // 2
    width = g_in.shape[1]
    zrows = g_in.shape[0] // line
    frows = zrows // 2
    up = {"fs": (f + 2) % (2 * line)}
    dn = {"fs": (f + 2 * line - 2) % (2 * line)}
    ypart = {"fs": f + 1 - 2 * y}
    xpart = {"rep": 1 - r}
    cpart = {"tp": 1 - core}

    barrier = pltpu.get_barrier_semaphore()
    for dev in (ypart, xpart, cpart, up, dn):
        pl.semaphore_signal(barrier, inc=1, device_id=dev, device_id_type=MESH)
    pl.semaphore_wait(barrier, 5)

    def remote(src, dst, s, q, dev):
        return pltpu.make_async_remote_copy(
            src_ref=src, dst_ref=dst, send_sem=s, recv_sem=q,
            device_id=dev, device_id_type=MESH,
        )

    def total(dst, terms, count, step=64):
        @pl.loop(0, count // step)
        def _(i):
            at = pl.multiple_of(i * step, step)
            value = None
            for ref, row, col, wide in terms:
                one = ref[pl.ds(row + at, step), pl.ds(col, wide)].astype(jnp.float32)
                value = one if value is None else value + one
            ref, row, col, wide = dst
            ref[pl.ds(row + at, step), pl.ds(col, wide)] = value.astype(ref.dtype)

    def slot(rr, yy):
        return pl.multiple_of((2 * rr + yy) * rows, rows)

    order = [(1 - r, 1 - y), (1 - r, y), (r, 1 - y), (r, y)]
    my_col = pl.multiple_of(core * cols, cols)
    its_col = pl.multiple_of((1 - core) * cols, cols)

    def core_copy(i):
        at = pl.ds(slot(*order[i]), rows)
        return remote(p_in.at[at, pl.ds(its_col, cols)], r1.at[at, :], c_s.at[i], c_r.at[i], cpart)

    def s1_half(i, second):
        return s1.at[pl.ds(slot(*order[i]), rows), pl.ds(side if second else 0, side)]

    def x_copy(i):
        src = (s1_half(0, False), s1_half(1, False), s3.at[1])[i]
        return remote(src, rx.at[i], x_s.at[i], x_r.at[i], xpart)

    def y_copy(i):
        src = (s1_half(0, True), s1_half(2, True), s3.at[0])[i]
        return remote(src, ry.at[i], yy_s.at[i], yy_r.at[i], ypart)

    def block(ref, zt):
        return ref.at[pl.ds(zt * zrows, zrows), :]

    def up_copy(zt, first):
        return remote(block(g_in if first else u_out, zt), block(u_in, zt), u_s.at[zt], u_r.at[zt], up)

    def dn_copy(zt, first):
        return remote(block(g_in if first else d_out, zt), block(d_in, zt), d_s.at[zt], d_r.at[zt], dn)

    def line_step(i):
        zt = line - 1 - i
        if zt > 0:
            @pl.when((z > 0) & (z < zt))
            def _():
                up_copy(zt, False).wait_recv()
                row = zt * zrows
                total((u_out, row, 0, width), [(g_in, row, 0, width), (u_in, row, 0, width)], zrows)
                up_copy(zt, False).start()

            zd = i

            @pl.when((z < line - 1) & (z > zd))
            def _():
                dn_copy(zd, False).wait_recv()
                row = zd * zrows
                total((d_out, row, 0, width), [(g_in, row, 0, width), (d_in, row, 0, width)], zrows)
                dn_copy(zd, False).start()

    def p_load(i):
        at = pl.ds(slot(*order[i]), rows)
        return pltpu.make_async_copy(p_in.at[at, pl.ds(my_col, cols)], p_tmp.at[at, :], loc.at[3 + i])

    for i in range(4):
        core_copy(i).start()
        p_load(i).start()
    for i in range(line - 1):
        @pl.when(z == 0)
        def _():
            up_copy(line - 1 - i, True).start()

        @pl.when(z == line - 1)
        def _():
            dn_copy(i, True).start()

    for i in range(4):
        p_load(i).wait()
        core_copy(i).wait_recv()
        row = slot(*order[i])
        total((s1, row, 0, cols), [(p_tmp, row, 0, cols), (r1, row, 0, cols)], rows)
        if i in (0, 1):
            x_copy(i).start()
        if i == 0:
            y_copy(0).start()
        if i == 2:
            y_copy(1).start()

    line_step(0)
    x_copy(0).wait_recv()
    total((s3.at[0], 0, 0, side), [(s1, slot(r, 1 - y), 0, side), (rx.at[0], 0, 0, side)], rows)
    y_copy(2).start()
    y_copy(0).wait_recv()
    total((s3.at[1], 0, 0, side), [(s1, slot(1 - r, y), side, side), (ry.at[0], 0, 0, side)], rows)
    x_copy(2).start()
    for i in range(1, line - 1):
        line_step(i)

    zrow = pl.multiple_of(z * zrows, zrows)

    def here(ref):
        return (ref, zrow, 0, width)

    @pl.when(z == 0)
    def _():
        dn_copy(0, True).wait_recv()
        total((gfin, 0, 0, width), [here(g_in), here(d_in)], zrows)

    @pl.when(z == line - 1)
    def _():
        up_copy(line - 1, True).wait_recv()
        total((gfin, 0, 0, width), [here(g_in), here(u_in)], zrows)

    @pl.when((z > 0) & (z < line - 1))
    def _():
        remote(block(g_in, z), block(u_in, z), u_s.at[z], u_r.at[z], up).wait_recv()
        remote(block(g_in, z), block(d_in, z), d_s.at[z], d_r.at[z], dn).wait_recv()
        total((gfin, 0, 0, width), [here(g_in), here(u_in), here(d_in)], zrows)

    def gcols(rr, yy):
        return gd_out.at[:, pl.ds(pl.multiple_of((2 * rr + yy) * width, width), width)]

    def grows(yy):
        return gfin.at[pl.ds(pl.multiple_of(yy * frows, frows), frows), :]

    def f_copy(i, landing):
        if i == 0:
            dst = gcols(r, 1 - y) if landing else gcols(r, y)
            return remote(grows(1 - y), dst, f_s.at[0], f_r.at[0], ypart)
        if i == 1:
            dst = gcols(1 - r, y) if landing else gcols(r, y)
            return remote(grows(y), dst, f_s.at[1], f_r.at[1], xpart)
        dst = gcols(1 - r, 1 - y) if landing else gcols(r, 1 - y)
        return remote(gcols(r, 1 - y), dst, f_s.at[2], f_r.at[2], xpart)

    f_copy(0, False).start()
    f_copy(1, False).start()
    own_g = pltpu.make_async_copy(grows(y), gcols(r, y), loc.at[0])
    own_g.start()

    x_copy(1).wait_recv()
    y_copy(2).wait_recv()
    here_row = slot(r, y)
    total(
        (fin, 0, 0, side),
        [(s1, here_row, 0, side), (rx.at[1], 0, 0, side), (ry.at[2], 0, 0, side)], rows,
    )

    def o_copy(i, landing):
        base = (1 - core if landing else core) * cols + i * side
        dst = gi_out.at[:, pl.ds(pl.multiple_of(base, side), side)]
        return remote(fin.at[:, pl.ds(i * side, side)], dst, o_s.at[i], o_r.at[i], cpart)

    def o_local(i):
        base = pl.multiple_of(core * cols + i * side, side)
        return pltpu.make_async_copy(
            fin.at[:, pl.ds(i * side, side)], gi_out.at[:, pl.ds(base, side)], loc.at[1 + i]
        )

    o_copy(0, False).start()
    o_local(0).start()
    f_copy(0, True).wait_recv()
    f_copy(2, False).start()
    y_copy(1).wait_recv()
    x_copy(2).wait_recv()
    total(
        (fin, 0, side, side),
        [(s1, here_row, side, side), (ry.at[1], 0, 0, side), (rx.at[2], 0, 0, side)], rows,
    )
    o_copy(1, False).start()
    o_local(1).start()

    for i in range(4):
        core_copy(i).wait_send()
    for i in range(3):
        x_copy(i).wait_send()
        y_copy(i).wait_send()
        f_copy(i, False).wait_send()
    f_copy(1, True).wait_recv()
    f_copy(2, True).wait_recv()
    for i in range(2):
        o_copy(i, True).wait_recv()
        o_copy(i, False).wait_send()
        o_local(i).wait()
    own_g.wait()
    for zt in range(line):
        if zt > 0:
            pl.when(z < zt)(lambda: up_copy(zt, True).wait_send())
        if zt < line - 1:
            pl.when(z > zt)(lambda: dn_copy(zt, True).wait_send())


def reduced(part, grad_part):
    line = lax.axis_size("fs") // 2
    rows, cols = part.shape[0] // 4, part.shape[1] // 2
    depth, width = grad_part.shape
    kind = part.dtype
    dma = pltpu.SemaphoreType.DMA
    vmem = pl.BlockSpec(memory_space=pltpu.VMEM)
    anyspec = pl.BlockSpec(memory_space=pl.ANY)
    unit = pltpu.VMEM((3, rows, cols // 2), kind)
    whole = pltpu.VMEM((depth, width), kind)
    return pl.pallas_call(
        functools.partial(reduce_kernel, line),
        out_shape=(
            jax.ShapeDtypeStruct((rows, 2 * cols), kind),
            jax.ShapeDtypeStruct((depth // (2 * line), 4 * width), kind),
        ),
        in_specs=[anyspec, vmem],
        out_specs=(anyspec, anyspec),
        scratch_shapes=[
            pltpu.VMEM((4 * rows, cols), kind),
            pltpu.VMEM((4 * rows, cols), kind),
            pltpu.VMEM((4 * rows, cols), kind),
            unit, unit,
            pltpu.VMEM((2, rows, cols // 2), kind),
            pltpu.VMEM((rows, cols), kind),
            whole, whole, whole, whole,
            pltpu.VMEM((depth // line, width), kind),
            dma((4,)), dma((4,)), dma((3,)), dma((3,)), dma((3,)), dma((3,)),
            dma((line,)), dma((line,)), dma((line,)), dma((line,)),
            dma((3,)), dma((3,)), dma((2,)), dma((2,)), dma((7,)),
        ],
        compiler_params=pltpu.CompilerParams(
            collective_id=1, has_side_effects=True, vmem_limit_bytes=56 * 2**20
        ),
        name="reduce_all",
    )(part, grad_part)


def on_device(inputs, cotangent, gate_weight, up_weight, down_weight):
    tok_rows = inputs.shape[0]
    fs_size = lax.axis_size("fs")
    rep_size = lax.axis_size("rep")
    contract = (((1,), (1,)), ((), ()))
    contract_tok = (((0,), (0,)), ((), ()))
    width = gate_weight.shape[1] // 4
    gate_up, down_full, tokens = gather(
        gate_weight, up_weight, down_weight, inputs, cotangent
    )
    gate_up_val = jnp.dot(tokens[0], gate_up, preferred_element_type=jnp.float32)
    gate_val, up_val = gate_up_val[:, :width], gate_up_val[:, width:]
    grad_hidden = jnp.dot(tokens[1], down_full, preferred_element_type=jnp.float32)
    sigmoid_gate = jax.nn.sigmoid(gate_val)
    active = gate_val * sigmoid_gate
    hidden = (active * up_val).astype(jnp.bfloat16)
    grad_gate = (
        grad_hidden * up_val * sigmoid_gate * (1.0 + gate_val * (1.0 - sigmoid_gate))
    ).astype(jnp.bfloat16)
    grad_up = (grad_hidden * active).astype(jnp.bfloat16)
    grad_scale = 1.0 / math.sqrt(tok_rows * fs_size * rep_size)
    pairs = [[i, i + 1] for i in range(0, fs_size, 2)]
    lines = [list(range(i, fs_size, 2)) for i in range(2)]
    grad_part = lax.dot_general(
        tokens[1], hidden, contract_tok, preferred_element_type=jnp.float32
    )
    part = lax.dot_general(
        jnp.concatenate([grad_gate, grad_up], axis=1), gate_up, contract,
        preferred_element_type=jnp.float32,
    )
    if lax.axis_size("tp") == 2:
        grad_input, grad_down = reduced(
            part.astype(jnp.bfloat16), grad_part.astype(jnp.bfloat16)
        )
        return (grad_input, grad_down.astype(jnp.float32) * grad_scale)
    shard = lax.psum_scatter(
        grad_part.astype(jnp.bfloat16), "fs", scatter_dimension=0, tiled=True,
        axis_index_groups=lines,
    ).astype(jnp.float32) * grad_scale
    shard = lax.all_to_all(
        shard, "fs", split_axis=0, concat_axis=1, tiled=True, axis_index_groups=pairs
    )
    grad_down = lax.all_gather(shard, "rep", axis=1, tiled=True)
    part = lax.psum_scatter(
        part.astype(jnp.bfloat16), "rep", scatter_dimension=0, tiled=True
    )
    part = lax.psum_scatter(
        part, "fs", scatter_dimension=0, tiled=True, axis_index_groups=pairs
    )
    grad_input = lax.psum(part, "tp")
    return (grad_input, grad_down)


def solution(mesh):
    placed = (
        P(("rep", "fs"), None),
        P(("rep", "fs"), None),
        P("fs", "tp"),
        P("fs", "tp"),
        P("fs", "tp"),
    )
    return jax.shard_map(
        on_device,
        mesh=mesh,
        in_specs=placed,
        out_specs=(P(("rep", "fs"), None), P("fs", "tp")),
        check_vma=False,
    )
```
